32 devices in a mesh: grp: 2 (over y), sp: 4 (over z), tp: 4 (over x, core).
Axes of the slice: x: 2, y: 2, z: 4, core: 2. Of those that a mesh axis runs over, the one named last changes fastest.
Arguments:
- skip_stream: bfloat16 [1024, 2048], P(('grp', 'sp', 'tp')), parts along dimension 0, may hold values from -6 to 6
- wide_probe_logits: bfloat16 [1024, 512], P(('grp', 'sp'), 'tp'), parts along dimension 0, may hold values from -6 to 6
- narrow_probe_logits: bfloat16 [1024, 512], P(('grp', 'sp'), 'tp'), parts along dimension 0, may hold values from -6 to 6
- wide_decay_logits: bfloat16 [1024, 512], P(('grp', 'sp'), 'tp'), parts along dimension 0, may hold values from -7.5 to 7.5
- narrow_decay_logits: bfloat16 [1024, 512], P(('grp', 'sp'), 'tp'), parts along dimension 0, may hold values from -7.5 to 7.5
- wide_floor_complement: float32 [2, 512], P(None, 'tp'), may hold values from 0.0002734375 to 0.21
- narrow_floor_complement: float32 [2, 512], P(None, 'tp'), may hold values from 0.0002734375 to 0.21
- payloads: bfloat16 [1024, 1536], P(('grp', 'sp'), 'tp'), parts along dimension 0, may hold values from -6 to 6
- result_switch_logits: bfloat16 [1024, 1536], P(('grp', 'sp'), 'tp'), parts along dimension 0, may hold values from -6 to 6
- spike_decays: float32 [1024, 12], P(('grp', 'sp'), 'tp'), parts along dimension 0, may hold values from -1.5 to 0
- channel_scale_vector: float32 [1536], P('tp'), may hold values from 0.1 to 1.9
- result_mapping_matrix: bfloat16 [1536, 2048], P('tp'), may hold values from -0.15625 to 0.15625
- specialist_scale_vector: float32 [2048], replicated, may hold values from 0.1 to 1.9
- assignments: int32 [1024, 2], P(('grp', 'sp', 'tp')), parts along dimension 0, may hold values from 0 to 3, all different within a row; in each aligned block of 32 rows (0 to 31, 32 to 63, ...) at most 32 rows name the same one
- assignment_share: float32 [1024, 2], P(('grp', 'sp', 'tp')), parts along dimension 0, may hold values from 0.2 to 1
- specialist_switch_matrix: bfloat16 [4, 2048, 3584], P('sp', None, 'tp'), may hold values from -0.125 to 0.125
- specialist_raising_matrix: bfloat16 [4, 2048, 3584], P('sp', None, 'tp'), may hold values from -0.125 to 0.125
- specialist_lowering_matrix: bfloat16 [4, 3584, 2048], P('sp', 'tp'), may hold values from -0.09375 to 0.09375
Outputs:
- layer_output: bfloat16 [1024, 2048], P(('grp', 'sp', 'tp')), parts along dimension 0
The draws below stay inside these ranges and needn't reach their ends.
There are 2 independent parts, one for each index of `grp`. The reference program is written for one: setup_inputs(seed, part) draws one part's arguments, and reference() takes and returns one part's arrays. A program takes and returns all parts, laid end to end along the dimension named above; an argument that names none is the same for every part. Nothing has to cross between parts.
Inputs may be any that keep to these rules, and one draw needn't show every extreme that they name: `assignments`: each row names 2 different experts; in each aligned block of 32 rows no expert is named by more than 32 rows, a bound that some block reaches.
All inputs are finite; a program needn't handle non-finite values.
Results may differ from the reference program's by a relative error of at most 0.015.
Values may be sent and summed in bfloat16 or wider, within the bound.
A program may use at most 128 MiB of HBM per device.

```python
import math
import jax
import jax.numpy as jnp
import numpy as np
from jax import lax

D = 2048
WIDE_GROUPS = 4
NARROW_GROUPS = 8
WIDE_LOOKUP_WIDTH = 128
NARROW_LOOKUP = 64
PAYLOAD_EXTENT = 128
DE = 3584
TOP = 2
BLOCK = 64
TOK_DEV = 128
ATTENTION_TALLY = 12
ELEMENT_TALLY = 512
ROWS = 32
EXPERTS = 4
DE_PART = 896
CAP = 32
N_SP = 4
N_TP = 4


def gate_draw(key, column_count, salt):
    noise_part = jnp.clip(jax.random.normal(jax.random.fold_in(key, salt), (ELEMENT_TALLY, column_count), jnp.float32), -6.0, 6.0)
    shifts = jax.random.uniform(jax.random.fold_in(key, salt + 1), (ELEMENT_TALLY // TOK_DEV, 1), jnp.float32, -1.5, 1.5)
    return (noise_part + jnp.repeat(shifts, TOK_DEV, axis=0)).astype(jnp.bfloat16)


def leak_draw(key, channel_tally, lookup_extent, salt):
    slow_limit = 5
    slow_heads = jax.random.randint(jax.random.fold_in(key, salt), (2, channel_tally, 1), 0, 10) < slow_limit
    slow_rate = jnp.exp(jax.random.uniform(jax.random.fold_in(key, salt + 1), (2, channel_tally, 1), jnp.float32, math.log(0.2), 0.0)) / ELEMENT_TALLY
    fast_rate = jnp.exp(jax.random.uniform(jax.random.fold_in(key, salt + 2), (2, channel_tally, 1), jnp.float32, math.log(0.03), math.log(0.15)))
    channel_spread = jnp.exp(jax.random.uniform(jax.random.fold_in(key, salt + 3), (2, channel_tally, lookup_extent), jnp.float32, math.log(0.7), math.log(1.4)))
    return (jnp.where(slow_heads, slow_rate, fast_rate) * channel_spread).reshape(2, channel_tally * lookup_extent)


def draw_wide_decay_logits(key, part):
    return gate_draw(key, WIDE_GROUPS * WIDE_LOOKUP_WIDTH, 101)


def draw_narrow_decay_logits(key, part):
    return gate_draw(key, NARROW_GROUPS * NARROW_LOOKUP, 201)


def draw_wide_floor_complement(key, part):
    return leak_draw(key, WIDE_GROUPS, WIDE_LOOKUP_WIDTH, 301)


def draw_narrow_floor_complement(key, part):
    return leak_draw(key, NARROW_GROUPS, NARROW_LOOKUP, 401)


def draw_spike_decays(key, part):
    spike_locations = jax.random.randint(jax.random.fold_in(key, 501), (3, ATTENTION_TALLY), 0, ELEMENT_TALLY)
    memory_extent = jax.random.uniform(jax.random.fold_in(key, 502), (3, ATTENTION_TALLY), jnp.float32, -0.5, -0.22)
    locations = jnp.arange(ELEMENT_TALLY, dtype=jnp.int32)[:, None, None]
    return jnp.sum(jnp.where(locations == spike_locations[None], memory_extent[None], 0.0), axis=1).astype(jnp.float32)


def level_of(own_key, extent, cuts, low, high):
    factor_of, own = 1.0, jax.random.fold_in(own_key, 6)
    for dim, parts in cuts:
        steps = jnp.exp(jax.random.uniform(jax.random.fold_in(own, dim), (parts,), jnp.float32, low / len(cuts), high / len(cuts)))
        factor_of = factor_of * jnp.repeat(steps, extent[dim] // parts).reshape([-1 if axis == dim else 1 for axis in range(len(extent))])
    return factor_of


def routed_block(key, own, number, rows, count, top, most, skew):
    order = jax.random.permutation(key, count)
    crowded, ordinary = shares(count, rows * top, most, skew, True), shares(count, rows * top, most, skew, False)
    places = jnp.arange(count)

    def named(lengths, turn):
        used = int((lengths > 0).sum())
        fixed = max(1, used // 4)
        shifted = fixed + (places - fixed + turn * (used - fixed)) % max(1, count - fixed)
        return jnp.zeros((count,), jnp.int32).at[order[jnp.where(places < fixed, places, shifted)]].set(jnp.asarray(lengths, jnp.int32))

    lengths = jnp.where(number % 4 == 0, named(crowded, number // 4), named(ordinary, number - number // 4 - 1))
    mixed = jax.random.permutation(jax.random.fold_in(own, 3), count)
    giver, sink = mixed[0:count // 2 * 2:2], mixed[1:count // 2 * 2:2]
    slack = jnp.minimum(lengths[giver] - 1, most - lengths[sink]) // 2
    slack = jnp.where((giver == order[0]) | (sink == order[0]) | (lengths[sink] == 0), 0, jnp.maximum(slack, 0))
    shifted = jax.random.randint(jax.random.fold_in(own, 4), (count // 2,), 0, 1 << 20) % (slack + 1)
    lengths = lengths.at[giver].add(-shifted).at[sink].add(shifted)
    members = jnp.searchsorted(jnp.cumsum(lengths), jnp.arange(rows * top), side="right").astype(jnp.int32)
    grid = members.reshape(top, rows).T
    grid = grid[jax.random.permutation(jax.random.fold_in(own, 1), rows)]
    turn = jax.random.randint(jax.random.fold_in(own, 2), (rows, 1), 0, top)
    return jnp.take_along_axis(grid, (jnp.arange(top)[None, :] + turn) % top, axis=1)


def shares(number_of, total, limit, slope, full):
    loads = [(1 << 20) // math.isqrt(rank ** slope) + 1 for rank in range(1, number_of + 1)]
    largest = limit if full else min(limit, max(-(-total // number_of), total * loads[0] // sum(loads)))
    least = 1 if total - largest >= number_of - 1 else 0
    given, spare = [largest] + [least] * (number_of - 1), total - largest - least * (number_of - 1)
    while spare > 0:
        movable = [i for i in range(1, number_of) if given[i] < largest] or [i for i in range(1, number_of) if given[i] < limit]
        pool, remaining = sum([loads[i] for i in movable]), spare
        for i in movable:
            addition = min(limit - given[i], max(1, remaining * loads[i] // pool), spare)
            given[i] = given[i] + addition
            spare = spare - addition
    return np.array(given)


def gaussian(rng, dims, scale, limit, cuts=(), held_as=jnp.bfloat16):
    gain = level_of(rng, dims, cuts, -0.22, 0.18) if cuts else 1.0
    entries = jax.random.normal(rng, dims, jnp.float32) * scale * gain
    return jnp.minimum(jnp.maximum(entries, -limit), limit).astype(held_as)


def setup_inputs(seed: int = 0, part: int = 0) -> dict:
    keys = jax.random.split(jax.random.key(seed), 19)
    part_splits = jax.random.split(jax.random.fold_in(keys[18], part), 19)
    skip_stream = gaussian(part_splits[0], (ELEMENT_TALLY, D), 1.0, 6.0, ((0, 16),))
    wide_probe_logits = gaussian(part_splits[1], (ELEMENT_TALLY, WIDE_GROUPS * WIDE_LOOKUP_WIDTH), 1.0, 6.0, ((0, 4), (1, 4)))
    narrow_probe_logits = gaussian(part_splits[2], (ELEMENT_TALLY, NARROW_GROUPS * NARROW_LOOKUP), 1.0, 6.0, ((0, 4), (1, 4)))
    wide_decay_logits = draw_wide_decay_logits(jax.random.fold_in(jax.random.fold_in(keys[18], part), 71), part)
    narrow_decay_logits = draw_narrow_decay_logits(jax.random.fold_in(jax.random.fold_in(keys[18], part), 71), part)
    wide_floor_complement = draw_wide_floor_complement(jax.random.fold_in(keys[18], 71), part)
    narrow_floor_complement = draw_narrow_floor_complement(jax.random.fold_in(keys[18], 71), part)
    payloads = gaussian(part_splits[7], (ELEMENT_TALLY, ATTENTION_TALLY * PAYLOAD_EXTENT), 1.0, 6.0, ((0, 4), (1, 4)))
    result_switch_logits = gaussian(part_splits[8], (ELEMENT_TALLY, ATTENTION_TALLY * PAYLOAD_EXTENT), 1.0, 6.0, ((0, 4), (1, 4)))
    spike_decays = draw_spike_decays(jax.random.fold_in(jax.random.fold_in(keys[18], part), 71), part)
    channel_scale_vector = jnp.clip(1.0 + 0.18 * jax.random.normal(keys[10], (ATTENTION_TALLY * PAYLOAD_EXTENT,), jnp.float32), 0.1, 1.9)
    result_mapping_matrix = gaussian(keys[11], (ATTENTION_TALLY * PAYLOAD_EXTENT, D), (ATTENTION_TALLY * PAYLOAD_EXTENT) ** -0.5, 0.15625, ((0, 4),))
    specialist_scale_vector = jnp.clip(1.0 + 0.18 * jax.random.normal(keys[12], (D,), jnp.float32), 0.1, 1.9)
    assignments_keys = jax.random.split(jax.random.fold_in(part_splits[13], 1), ELEMENT_TALLY // ROWS)
    assignments_turns = jax.random.permutation(jax.random.fold_in(part_splits[13], 3), ELEMENT_TALLY // ROWS)
    assignments = jax.vmap(lambda own, number: routed_block(jax.random.fold_in(part_splits[13], 2), own, number, ROWS, EXPERTS, TOP, CAP, 2))(assignments_keys, assignments_turns).reshape((ELEMENT_TALLY, TOP))
    assignment_share = jnp.clip(0.2 + 0.8 * jax.random.uniform(part_splits[14], (ELEMENT_TALLY, TOP), jnp.float32) ** level_of(part_splits[14], (ELEMENT_TALLY, TOP), ((0, 16),), -0.2, 0.2), 0.2, 1.0)
    specialist_switch_matrix = gaussian(keys[15], (EXPERTS, D, DE), D ** -0.5, 0.125, ((0, 4), (2, 4)))
    specialist_raising_matrix = gaussian(keys[16], (EXPERTS, D, DE), D ** -0.5, 0.125, ((0, 4), (2, 4)))
    specialist_lowering_matrix = gaussian(keys[17], (EXPERTS, DE, D), DE ** -0.5, 0.09375, ((0, 4), (1, 4)))
    return dict(skip_stream=skip_stream, wide_probe_logits=wide_probe_logits, narrow_probe_logits=narrow_probe_logits, wide_decay_logits=wide_decay_logits, narrow_decay_logits=narrow_decay_logits, wide_floor_complement=wide_floor_complement, narrow_floor_complement=narrow_floor_complement, payloads=payloads, result_switch_logits=result_switch_logits, spike_decays=spike_decays, channel_scale_vector=channel_scale_vector, result_mapping_matrix=result_mapping_matrix, specialist_scale_vector=specialist_scale_vector, assignments=assignments, assignment_share=assignment_share, specialist_switch_matrix=specialist_switch_matrix, specialist_raising_matrix=specialist_raising_matrix, specialist_lowering_matrix=specialist_lowering_matrix)


epsilon = 1e-06

def switch_cumulants(decay_factor, floor_complement, spike_log_decay):
    initial_memory = jax.nn.sigmoid(-decay_factor)
    key_input = floor_complement * initial_memory
    keep_log_decay = jnp.log1p(-floor_complement * initial_memory) + spike_log_decay[:, :, None]
    return (key_input, keep_log_decay)

def block_pass(queries, key_input, memory_matrix, keep_log_decay, initial):
    series_extent = queries.shape[0]
    channel_tally = queries.shape[1]
    block_count = series_extent // BLOCK

    def to_blocks(tensor):
        return tensor.reshape(block_count, BLOCK, channel_tally, tensor.shape[-1]).transpose(0, 2, 1, 3)
    below_mask = jnp.tril(jnp.ones((BLOCK, BLOCK), dtype=bool))[None, :, :, None]

    def advance(carried, segment):
        query_block, key_block, value_block, decay_block = segment
        running = jnp.cumsum(decay_block, axis=1)
        log_gap = running[:, :, None, :] - running[:, None, :, :]
        weight = jnp.where(below_mask, jnp.exp(jnp.where(below_mask, log_gap, 0.0)), 0.0)
        scores = jnp.einsum('htd,hsd,htsd->hts', query_block, key_block, weight, precision=lax.Precision.HIGHEST)
        output = jnp.einsum('hts,hse->hte', scores, value_block, precision=lax.Precision.HIGHEST)
        output = output + jnp.einsum('htd,hde->hte', query_block * jnp.exp(running), carried, precision=lax.Precision.HIGHEST)
        closing = running[:, -1:, :]
        fresh = jnp.einsum('hsd,hse->hde', key_block * jnp.exp(closing - running), value_block, precision=lax.Precision.HIGHEST)
        carried = jnp.exp(closing[:, 0, :, None]) * carried + fresh
        return (carried, output)
    closing_state, outputs = lax.scan(advance, initial, (to_blocks(queries), to_blocks(key_input), to_blocks(memory_matrix), to_blocks(keep_log_decay)))
    return (outputs.transpose(0, 2, 1, 3).reshape(series_extent, channel_tally, -1), closing_state)

def twin_orientations(probe_logits, decay_factor, floor_complement, spike_log_decay, memory_matrix, lookup_extent):
    series_extent = probe_logits.shape[0]
    channel_tally = spike_log_decay.shape[1]
    queries = jax.nn.silu(probe_logits.astype(jnp.float32).reshape(series_extent, channel_tally, lookup_extent)) * lookup_extent ** (-0.5)
    decay_switch_level = decay_factor.astype(jnp.float32).reshape(series_extent, channel_tally, lookup_extent)
    initial = jnp.zeros((channel_tally, lookup_extent, memory_matrix.shape[-1]), jnp.float32)
    onward_lookup, onward_log_decay = switch_cumulants(decay_switch_level, floor_complement[0].reshape(channel_tally, lookup_extent), spike_log_decay)
    reverse_lookup, reverse_log_decay = switch_cumulants(decay_switch_level, floor_complement[1].reshape(channel_tally, lookup_extent), spike_log_decay)
    ahead = block_pass(queries, onward_lookup, memory_matrix, onward_log_decay, initial)[0]
    behind = block_pass(jnp.flip(queries, axis=0), jnp.flip(reverse_lookup, axis=0), jnp.flip(memory_matrix, axis=0), jnp.flip(reverse_log_decay, axis=0), initial)[0]
    return ahead + jnp.flip(behind, axis=0)

def reference(skip_stream, wide_probe_logits, narrow_probe_logits, wide_decay_logits, narrow_decay_logits, wide_floor_complement, narrow_floor_complement, payloads, result_switch_logits, spike_decays, channel_scale_vector, result_mapping_matrix, specialist_scale_vector, assignments, assignment_share, specialist_switch_matrix, specialist_raising_matrix, specialist_lowering_matrix):
    series_extent = skip_stream.shape[0]
    joint_heads = 3 * WIDE_GROUPS
    memory_matrix = payloads.astype(jnp.float32).reshape(series_extent, WIDE_GROUPS, 3, PAYLOAD_EXTENT)
    spike_span = spike_decays.reshape(series_extent, WIDE_GROUPS, 3)
    wide_channel_slices = twin_orientations(wide_probe_logits, wide_decay_logits, wide_floor_complement, spike_span[:, :, 0], memory_matrix[:, :, 0], WIDE_LOOKUP_WIDTH)
    narrow_channel_slices = twin_orientations(narrow_probe_logits, narrow_decay_logits, narrow_floor_complement, spike_span[:, :, 1:].reshape(series_extent, NARROW_GROUPS), memory_matrix[:, :, 1:].reshape(series_extent, NARROW_GROUPS, PAYLOAD_EXTENT), NARROW_LOOKUP)
    joined = jnp.concatenate([wide_channel_slices[:, :, None], narrow_channel_slices.reshape(series_extent, WIDE_GROUPS, 2, PAYLOAD_EXTENT)], axis=2).reshape(series_extent, joint_heads, PAYLOAD_EXTENT)
    normed_heads = joined * lax.rsqrt(lax.optimization_barrier(jnp.mean(joined * joined, axis=-1, keepdims=True)) + epsilon)
    gated_heads = normed_heads * channel_scale_vector.reshape(joint_heads, PAYLOAD_EXTENT) * jax.nn.silu(result_switch_logits.astype(jnp.float32).reshape(series_extent, joint_heads, PAYLOAD_EXTENT))
    mixed_heads = gated_heads.reshape(series_extent, joint_heads * PAYLOAD_EXTENT).astype(jnp.bfloat16)
    mixing = jnp.dot(mixed_heads, result_mapping_matrix, preferred_element_type=jnp.float32)
    hidden = (skip_stream.astype(jnp.float32) + mixing).astype(jnp.bfloat16)
    hidden_float = hidden.astype(jnp.float32)
    normed = (hidden_float * lax.rsqrt(lax.optimization_barrier(jnp.mean(hidden_float * hidden_float, axis=-1, keepdims=True)) + epsilon) * specialist_scale_vector).astype(jnp.bfloat16)
    most_rows = N_SP * N_TP * CAP
    block_total = DE // DE_PART

    def one_expert(running_sum, expert_index):
        chosen = assignments == expert_index
        weight_share = lax.optimization_barrier(jnp.sum(jnp.where(chosen, assignment_share, 0.0), axis=1))
        used_rows = jnp.any(chosen, axis=1)
        picked = jnp.nonzero(used_rows, size=most_rows, fill_value=0)[0].astype(jnp.int32)
        live_rows = jnp.arange(most_rows, dtype=jnp.int32) < jnp.sum(used_rows.astype(jnp.int32))
        gathered = normed[picked]
        gate_part = jnp.dot(gathered, specialist_switch_matrix[expert_index], preferred_element_type=jnp.float32)
        up_part = jnp.dot(gathered, specialist_raising_matrix[expert_index], preferred_element_type=jnp.float32)
        activation = (jax.nn.silu(gate_part) * up_part).astype(jnp.bfloat16)
        partial_value = jnp.einsum('mpk,pkd->mpd', activation.astype(jnp.float32).reshape(most_rows, block_total, DE_PART), specialist_lowering_matrix[expert_index].astype(jnp.float32).reshape(block_total, DE_PART, D), precision=lax.Precision.HIGHEST)
        rounded = lax.optimization_barrier(partial_value.astype(jnp.bfloat16)).astype(jnp.float32)
        expert_out = lax.optimization_barrier(jnp.sum(rounded, axis=1)).astype(jnp.bfloat16)
        row_scale = jnp.where(live_rows, weight_share[picked], 0.0)
        running_sum = running_sum.at[picked].add(row_scale[:, None] * expert_out.astype(jnp.float32))
        return (running_sum, None)
    mixture = lax.scan(one_expert, jnp.zeros((series_extent, D), jnp.float32), jnp.arange(EXPERTS, dtype=jnp.int32))[0]
    return (hidden_float + mixture).astype(jnp.bfloat16)
```

```python
import functools

import jax
import jax.numpy as jnp
from jax import lax
from jax.experimental import pallas as pl
from jax.experimental.pallas import tpu as pltpu
from jax.sharding import PartitionSpec as P

LANES = 128
NEAR = 2
EPS = 1e-06
F32 = jnp.float32
BF16 = jnp.bfloat16


def mm(a, b, ca=1, cb=0):
    return lax.dot_general(a, b, (((ca,), (cb,)), ((), ())), preferred_element_type=F32)


def kernel(
    n_sp,
    n_tp,
    cap,
    capp,
    skip_ref,
    wq_ref,
    nq_ref,
    wf_ref,
    nf_ref,
    wl_ref,
    nl_ref,
    v_ref,
    gate_ref,
    spk_ref,
    chs_ref,
    wo_hbm,
    nsc_ref,
    asg_ref,
    shr_ref,
    wg_hbm,
    wu_hbm,
    wd_hbm,
    out_ref,
    wo,
    wg,
    wu,
    wd,
    st_out,
    st_in,
    y_s,
    rs_out,
    rs_in,
    hid_s,
    disp,
    xin,
    part,
    nr_in,
    fr_out,
    fr_in,
    fin,
    ret,
    wsem,
    st_ss,
    st_rs,
    rs_ss,
    rs_rs,
    z_ss,
    far_ss,
    near_ss,
    ag_rs,
    nr_ss,
    nr_rs,
    fr_ss,
    fr_rs,
    ret_ss,
    ret_rs,
):
    sp = lax.axis_index("sp")
    tp = lax.axis_index("tp")
    n_hi = n_tp // NEAR
    hi = tp // NEAR
    near = tp + 1 - 2 * (tp % NEAR)
    near_lo = near % NEAR
    lo = tp % NEAR
    rows = skip_ref.shape[0]
    L = wq_ref.shape[0]
    H = L // 2
    group = n_tp * capp

    def al(i):
        return pl.multiple_of(i * capp, capp)

    weights = [
        pltpu.make_async_copy(wo_hbm, wo, wsem.at[0]),
        pltpu.make_async_copy(wg_hbm.at[0], wg, wsem.at[1]),
        pltpu.make_async_copy(wu_hbm.at[0], wu, wsem.at[2]),
        pltpu.make_async_copy(wd_hbm.at[0], wd, wsem.at[3]),
    ]
    for w in weights:
        w.start()

    barrier = pltpu.get_barrier_semaphore()
    for o in range(1, n_sp):
        pl.semaphore_signal(barrier, inc=1, device_id={"sp": (sp + o) % n_sp})
    for o in range(1, n_tp):
        pl.semaphore_signal(barrier, inc=1, device_id={"tp": (tp + o) % n_tp})

    lane = lax.broadcasted_iota(jnp.int32, (1, LANES), 1)
    first = lane < LANES // 2
    spk = spk_ref[...]
    spike = jnp.concatenate(
        [
            jnp.broadcast_to(spk[:, 0:1], (L, LANES)),
            jnp.where(first, spk[:, 1:2], spk[:, 2:3]),
        ],
        axis=1,
    )
    forget = jnp.concatenate([wf_ref[...], nf_ref[...]], axis=1).astype(F32)
    start = 1.0 / (1.0 + jnp.exp(forget))
    wq = wq_ref[...].astype(F32)
    nq = nq_ref[...].astype(F32)
    q = jnp.concatenate(
        [
            wq / (1.0 + jnp.exp(-wq)) * LANES**-0.5,
            nq / (1.0 + jnp.exp(-nq)) * (LANES // 2) ** -0.5,
        ],
        axis=1,
    )
    leak = jnp.concatenate([wl_ref[...], nl_ref[...]], axis=1)
    t_i = lax.broadcasted_iota(jnp.int32, (L, L), 0)
    s_i = lax.broadcasted_iota(jnp.int32, (L, L), 1)
    row = lax.broadcasted_iota(jnp.int32, (L, 1), 0)
    past = s_i <= t_i
    later = s_i >= t_i
    same = (t_i < H) == (s_i < H)
    v = v_ref[...]
    vs = [v[:, h * LANES : (h + 1) * LANES] for h in range(3)]
    ks, runs = [], []
    for d in range(2):
        k = leak[d : d + 1, :] * start
        a = jnp.log(1.0 - k) + spike
        tri = (past if d == 0 else later).astype(F32)
        run = lax.dot_general(
            tri,
            a,
            (((1,), (0,)), ((), ())),
            preferred_element_type=F32,
            precision=lax.Precision.HIGHEST,
        )
        total = run[L - 1 : L, :] if d == 0 else run[0:1, :]
        kk = (k * jnp.exp(total - run)).astype(BF16)
        wide = mm(vs[0], kk[:, :LANES], 0, 0)
        slim = jnp.where(first, mm(vs[1], kk[:, LANES:], 0, 0), mm(vs[2], kk[:, LANES:], 0, 0))
        st_out[d, :LANES, :] = jnp.concatenate([wide, slim], axis=1).astype(BF16)
        st_out[d, LANES:, :] = jnp.broadcast_to(
            total, (st_out.shape[1] - LANES, 2 * LANES)
        ).astype(BF16)
        ks.append(k)
        runs.append(run)

    pl.semaphore_wait(barrier, n_sp + n_tp - 2)

    def st_copy(o):
        dest = (sp + o) % n_sp
        way = (sp + o) // n_sp
        return pltpu.make_async_remote_copy(
            src_ref=st_out.at[way],
            dst_ref=st_in.at[sp],
            send_sem=st_ss.at[o],
            recv_sem=st_rs.at[sp],
            device_id={"sp": dest},
        )

    for o in range(1, n_sp):
        st_copy(o).start()

    outs = []
    scores = [None, None, None]
    for d in range(2):
        k, run = ks[d], runs[d]
        mid = jnp.where(row < H, run[H // 2 - 1 : H // 2, :], run[H + H // 2 - 1 : H + H // 2, :])
        edge = run[H - 1 : H, :] if d == 0 else run[H : H + 1, :]
        q_in = q * jnp.exp(run - mid)
        k_in = (k * jnp.exp(mid - run)).astype(BF16)
        q_off = q * jnp.exp(jnp.minimum(run - edge, 0.0))
        k_off = (k * jnp.exp(jnp.minimum(edge - run, 0.0))).astype(BF16)
        keep_in = same & (past if d == 0 else later)
        keep_off = ((t_i >= H) & (s_i < H)) if d == 0 else ((t_i < H) & (s_i >= H))
        for h in range(3):
            at = slice(0, LANES) if h == 0 else slice(LANES, 2 * LANES)
            qi, qo = q_in[:, at], q_off[:, at]
            if h > 0:
                mine = first if h == 1 else ~first
                qi, qo = jnp.where(mine, qi, 0.0), jnp.where(mine, qo, 0.0)
            part_in = jnp.where(keep_in, mm(qi.astype(BF16), k_in[:, at], 1, 1), 0.0)
            part_off = jnp.where(keep_off, mm(qo.astype(BF16), k_off[:, at], 1, 1), 0.0)
            both = part_in + part_off
            scores[h] = both if d == 0 else scores[h] + both
    for h in range(3):
        outs.append(mm(scores[h].astype(BF16), vs[h]))

    def take(src, state):
        pltpu.make_async_remote_copy(
            src_ref=st_out.at[0],
            dst_ref=st_in.at[src],
            send_sem=st_ss.at[0],
            recv_sem=st_rs.at[src],
            device_id={"sp": (sp + 1) % n_sp},
        ).wait_recv()
        got = st_in[src].astype(F32)
        return state * jnp.exp(got[LANES : LANES + 1, :]) + got[:LANES, :]

    zero = jnp.zeros((LANES, 2 * LANES), F32)
    ahead = lax.fori_loop(0, sp, take, zero)
    behind = lax.fori_loop(0, n_sp - 1 - sp, lambda i, s: take(n_sp - 1 - i, s), zero)
    for d, state in enumerate((ahead, behind)):
        state = state.astype(BF16)
        qd = q * jnp.exp(runs[d])
        for h in range(3):
            at = slice(0, LANES) if h == 0 else slice(LANES, 2 * LANES)
            qh = qd[:, at]
            if h > 0:
                qh = jnp.where(first if h == 1 else ~first, qh, 0.0)
            outs[h] = outs[h] + mm(qh.astype(BF16), state[:, at], 1, 1)
    g = gate_ref[...].astype(F32)
    g = g / (1.0 + jnp.exp(-g)) * chs_ref[...]
    for h in range(3):
        at = slice(h * LANES, (h + 1) * LANES)
        o_h = outs[h]
        o_h = o_h * lax.rsqrt(jnp.mean(o_h * o_h, axis=1, keepdims=True) + EPS)
        y_s[:, at] = (o_h * g[:, at]).astype(BF16)

    weights[0].wait()
    y = y_s[...]
    D = wo.shape[1]
    step = D // 4
    for c in range(4):
        rs_out[:, c * step : (c + 1) * step] = mm(y, wo[:, c * step : (c + 1) * step]).astype(BF16)

    def rs_copy(o):
        dest = (tp + o) % n_tp
        return pltpu.make_async_remote_copy(
            src_ref=rs_out.at[pl.ds(pl.multiple_of(dest * rows, rows), rows)],
            dst_ref=rs_in.at[o - 1],
            send_sem=rs_ss.at[o - 1],
            recv_sem=rs_rs.at[o - 1],
            device_id={"tp": dest},
        )

    for o in range(1, n_tp):
        rs_copy(o).start()

    n_slot = n_sp * capp
    slot = lax.broadcasted_iota(jnp.int32, (1, n_slot), 1)
    expert = jnp.zeros((1, n_slot), jnp.int32)
    for e in range(1, n_sp):
        expert = expert + (slot >= e * capp).astype(jnp.int32)
    place = (slot - expert * capp).astype(F32)
    asg = asg_ref[...]
    shr = shr_ref[...]
    named = jnp.zeros((rows, n_slot), F32)
    share = jnp.zeros((rows, n_slot), F32)
    for c in range(asg.shape[1]):
        hit = asg[:, c : c + 1] == expert
        named = jnp.where(hit, 1.0, named)
        share = jnp.where(hit, shr[:, c : c + 1], share)
    before = (
        lax.broadcasted_iota(jnp.int32, (rows, rows), 1)
        < lax.broadcasted_iota(jnp.int32, (rows, rows), 0)
    ).astype(BF16)
    count = mm(before, named.astype(BF16))
    picked = jnp.where(count == place, named, 0.0)
    comb = picked * share
    comb_hi = comb.astype(BF16)
    comb_lo = (comb - comb_hi.astype(F32)).astype(BF16)

    total = skip_ref[...].astype(F32) + rs_out[pl.ds(pl.multiple_of(tp * rows, rows), rows), :].astype(F32)
    for o in range(1, n_tp):
        rs_copy(o).wait_recv()
        total = total + rs_in[o - 1].astype(F32)
    hid = total.astype(BF16)
    hid_s[...] = hid
    hf = hid.astype(F32)
    normed = (
        hf * lax.rsqrt(jnp.mean(hf * hf, axis=1, keepdims=True) + EPS) * nsc_ref[...]
    ).astype(BF16)
    disp[...] = mm(picked.astype(BF16), normed, 0, 0).astype(BF16)

    def chunk(src, t):
        return al(src * n_tp + t)

    def z_copy(o):
        dest = (sp + o) % n_sp
        return pltpu.make_async_remote_copy(
            src_ref=disp.at[pl.ds(al(dest), capp)],
            dst_ref=xin.at[pl.ds(chunk(sp, tp), capp)],
            send_sem=z_ss.at[o],
            recv_sem=ag_rs.at[sp, tp],
            device_id={"sp": dest},
        )

    for o in range(1, n_sp):
        z_copy(o).start()
    xin[pl.ds(chunk(sp, tp), capp), :] = disp[pl.ds(al(sp), capp), :]

    def source(i):
        return (sp + i) % n_sp

    def tp_copy(src, t, sem, dest):
        return pltpu.make_async_remote_copy(
            src_ref=xin.at[pl.ds(chunk(src, t), capp)],
            dst_ref=xin.at[pl.ds(chunk(src, t), capp)],
            send_sem=sem,
            recv_sem=ag_rs.at[src, t],
            device_id={"tp": dest},
        )

    def far_copy(i, h):
        return tp_copy(source(i), tp, far_ss.at[i, h], (tp + NEAR * h) % n_tp)

    def near_copy(i, h):
        return tp_copy(source(i), (tp + NEAR * h) % n_tp, near_ss.at[i, h], near)

    def arrived(i, t):
        tp_copy(source(i), t, near_ss.at[i, 0], near).wait_recv()

    def spread(i):
        for h in range(1, n_hi):
            far_copy(i, h).start()
        near_copy(i, 0).start()

    def relay(i):
        for h in range(1, n_hi):
            arrived(i, (tp + NEAR * h) % n_tp)
            near_copy(i, h).start()

    def nr_copy(i, h):
        src = source(i)
        return pltpu.make_async_remote_copy(
            src_ref=part.at[pl.ds(chunk(src, h * NEAR + near_lo), capp)],
            dst_ref=nr_in.at[pl.ds(al(src * n_hi + h), capp)],
            send_sem=nr_ss.at[i, h],
            recv_sem=nr_rs.at[src, h],
            device_id={"tp": near},
        )

    def fr_copy(i, o):
        src = source(i)
        h = (hi + o) % n_hi
        return pltpu.make_async_remote_copy(
            src_ref=fr_out.at[pl.ds(al(src * n_hi + h), capp)],
            dst_ref=fr_in.at[pl.ds(al(src * n_hi + o), capp)],
            send_sem=fr_ss.at[i, o],
            recv_sem=fr_rs.at[src, o],
            device_id={"tp": (tp + NEAR * o) % n_tp},
        )

    def ret_copy(i):
        src = source(i)
        return pltpu.make_async_remote_copy(
            src_ref=fin.at[pl.ds(al(src), capp)],
            dst_ref=ret.at[pl.ds(al(sp), capp)],
            send_sem=ret_ss.at[i],
            recv_sem=ret_rs.at[sp],
            device_id={"sp": src},
        )

    def ffn(i):
        src = source(i)
        for h in range(n_hi):
            arrived(i, (near + NEAR * h) % n_tp)
        at = pl.multiple_of(src * group, group)
        x = xin[pl.ds(at, group), :]
        gp = mm(x, wg[...])
        up = mm(x, wu[...])
        act = (gp / (1.0 + jnp.exp(-gp)) * up).astype(BF16)
        for c in range(4):
            part[pl.ds(at, group), c * step : (c + 1) * step] = mm(
                act, wd[:, c * step : (c + 1) * step]
            ).astype(BF16)
        for h in range(n_hi):
            nr_copy(i, h).start()

    def near_sum(i):
        src = source(i)
        for o in range(1, n_hi + 1):
            h = (hi + o) % n_hi
            nr_copy(i, h).wait_recv()
            slot_at = pl.ds(al(src * n_hi + h), capp)
            fr_out[slot_at, :] = (
                part[pl.ds(chunk(src, h * NEAR + lo), capp), :].astype(F32)
                + nr_in[slot_at, :].astype(F32)
            ).astype(BF16)
            if o < n_hi:
                fr_copy(i, o).start()

    def far_sum(i):
        src = source(i)
        acc = fr_out[pl.ds(al(src * n_hi + hi), capp), :].astype(F32)
        for o in range(1, n_hi):
            fr_copy(i, o).wait_recv()
            acc = acc + fr_in[pl.ds(al(src * n_hi + o), capp), :].astype(F32)
        fin[pl.ds(al(src), capp), :] = acc.astype(BF16)

    spread(0)
    relay(0)
    for w in weights[1:]:
        w.wait()

    def z_arrived(i):
        src = source(i)
        pltpu.make_async_remote_copy(
            src_ref=disp.at[pl.ds(0, capp)],
            dst_ref=xin.at[pl.ds(chunk(src, tp), capp)],
            send_sem=z_ss.at[0],
            recv_sem=ag_rs.at[src, tp],
            device_id={"sp": (sp + 1) % n_sp},
        ).wait_recv()

    if n_sp > 1:
        z_arrived(1)
        spread(1)

    def body(i, carry):
        @pl.when(i < n_sp)
        def _():
            ffn(i)

        @pl.when(i + 1 < n_sp)
        def _():
            relay(i + 1)

        @pl.when(i + 2 < n_sp)
        def _():
            z_arrived(i + 2)
            spread(i + 2)

        @pl.when((i >= 1) & (i <= n_sp))
        def _():
            near_sum(i - 1)

        @pl.when(i >= 2)
        def _():
            far_sum(i - 2)

        @pl.when(i >= 3)
        def _():
            ret_copy(i - 2).start()

        return carry

    lax.fori_loop(0, n_sp + 2, body, 0)

    ret[pl.ds(al(sp), capp), :] = fin[pl.ds(al(sp), capp), :]
    for o in range(1, n_sp):
        src = (sp + o) % n_sp
        pltpu.make_async_remote_copy(
            src_ref=fin.at[pl.ds(0, capp)],
            dst_ref=ret.at[pl.ds(al(src), capp)],
            send_sem=ret_ss.at[0],
            recv_sem=ret_rs.at[src],
            device_id={"sp": src},
        ).wait_recv()
    back = ret[...]
    out_ref[...] = (hid_s[...].astype(F32) + mm(comb_hi, back) + mm(comb_lo, back)).astype(BF16)

    for o in range(1, n_sp):
        st_copy(o).wait_send()
        z_copy(o).wait_send()
        ret_copy(o).wait_send()
    for o in range(1, n_tp):
        rs_copy(o).wait_send()

    def drain(i, carry):
        for h in range(1, n_hi):
            far_copy(i, h).wait_send()
            fr_copy(i, h).wait_send()
        for h in range(n_hi):
            near_copy(i, h).wait_send()
            nr_copy(i, h).wait_send()
        return carry

    lax.fori_loop(0, n_sp, drain, 0)


def local(n_sp, n_tp, *args):
    skip, wq = args[0], args[1]
    rows, D = skip.shape
    L = wq.shape[0]
    top = args[13].shape[1]
    cap = max(2, 2 * rows * top // n_sp)
    cap = min(cap, rows)
    capp = -(-cap // 16) * 16
    n_hi = n_tp // NEAR
    de = args[15].shape[2]
    heads = args[11].shape[0]
    args = list(args)
    args[10] = args[10].reshape(1, -1)
    args[12] = args[12].reshape(1, -1)
    vm = pl.BlockSpec(memory_space=pltpu.VMEM)
    hbm = pl.BlockSpec(memory_space=pl.ANY)
    specs = [hbm if i in (11, 15, 16, 17) else vm for i in range(len(args))]
    dma = pltpu.SemaphoreType.DMA
    scratch = [
        pltpu.VMEM((heads, D), BF16),
        pltpu.VMEM((D, de), BF16),
        pltpu.VMEM((D, de), BF16),
        pltpu.VMEM((de, D), BF16),
        pltpu.VMEM((2, LANES + 16, 2 * LANES), BF16),
        pltpu.VMEM((n_sp, LANES + 16, 2 * LANES), BF16),
        pltpu.VMEM((L, heads), BF16),
        pltpu.VMEM((L, D), BF16),
        pltpu.VMEM((n_tp - 1, rows, D), BF16),
        pltpu.VMEM((rows, D), BF16),
        pltpu.VMEM((n_sp * capp, D), BF16),
        pltpu.VMEM((n_sp * n_tp * capp, D), BF16),
        pltpu.VMEM((n_sp * n_tp * capp, D), BF16),
        pltpu.VMEM((n_sp * n_hi * capp, D), BF16),
        pltpu.VMEM((n_sp * n_hi * capp, D), BF16),
        pltpu.VMEM((n_sp * n_hi * capp, D), BF16),
        pltpu.VMEM((n_sp * capp, D), BF16),
        pltpu.VMEM((n_sp * capp, D), BF16),
        dma((4,)),
        dma((n_sp,)),
        dma((n_sp,)),
        dma((n_tp - 1,)),
        dma((n_tp - 1,)),
        dma((n_sp,)),
        dma((n_sp, n_hi)),
        dma((n_sp, n_hi)),
        dma((n_sp, n_tp)),
        dma((n_sp, n_hi)),
        dma((n_sp, n_hi)),
        dma((n_sp, n_hi)),
        dma((n_sp, n_hi)),
        dma((n_sp,)),
        dma((n_sp,)),
    ]
    return pl.pallas_call(
        functools.partial(kernel, n_sp, n_tp, cap, capp),
        out_shape=jax.ShapeDtypeStruct((rows, D), BF16),
        in_specs=specs,
        out_specs=vm,
        scratch_shapes=scratch,
        compiler_params=pltpu.CompilerParams(
            collective_id=0, has_side_effects=True, vmem_limit_bytes=60 * 1024 * 1024
        ),
    )(*args)


def solution(mesh):
    placed = (
        P(("grp", "sp", "tp"), None),
        P(("grp", "sp"), "tp"),
        P(("grp", "sp"), "tp"),
        P(("grp", "sp"), "tp"),
        P(("grp", "sp"), "tp"),
        P(None, "tp"),
        P(None, "tp"),
        P(("grp", "sp"), "tp"),
        P(("grp", "sp"), "tp"),
        P(("grp", "sp"), "tp"),
        P("tp"),
        P("tp", None),
        P(),
        P(("grp", "sp", "tp"), None),
        P(("grp", "sp", "tp"), None),
        P("sp", None, "tp"),
        P("sp", None, "tp"),
        P("sp", "tp", None),
    )
    return jax.shard_map(
        functools.partial(local, mesh.shape["sp"], mesh.shape["tp"]),
        mesh=mesh,
        in_specs=placed,
        out_specs=P(("grp", "sp", "tp"), None),
        check_vma=False,
    )
```

```python
import functools

import jax
import jax.numpy as jnp
from jax import lax
from jax.experimental import pallas as pl
from jax.experimental.pallas import tpu as pltpu
from jax.sharding import PartitionSpec as P

LANES = 128
NEAR = 2
EPS = 1e-06
F32 = jnp.float32
BF16 = jnp.bfloat16


def mm(a, b, ca=1, cb=0):
    return lax.dot_general(a, b, (((ca,), (cb,)), ((), ())), preferred_element_type=F32)


def kernel(
    n_sp,
    n_tp,
    cap,
    capp,
    skip_ref,
    wq_ref,
    nq_ref,
    wf_ref,
    nf_ref,
    wl_ref,
    nl_ref,
    v_ref,
    gate_ref,
    spk_ref,
    chs_ref,
    wo_hbm,
    nsc_ref,
    asg_ref,
    shr_ref,
    wg_hbm,
    wu_hbm,
    wd_hbm,
    out_ref,
    wo,
    wg,
    wu,
    wd,
    st_out,
    st_in,
    y_s,
    rs_out,
    rs_in,
    hid_s,
    disp,
    xin,
    part,
    nr_in,
    fr_out,
    fr_in,
    fin,
    ret,
    wsem,
    st_ss,
    st_rs,
    rs_ss,
    rs_rs,
    z_ss,
    far_ss,
    near_ss,
    ag_rs,
    nr_ss,
    nr_rs,
    fr_ss,
    fr_rs,
    ret_ss,
    ret_rs,
):
    sp = lax.axis_index("sp")
    tp = lax.axis_index("tp")
    n_hi = n_tp // NEAR
    hi = tp // NEAR
    near = tp + 1 - 2 * (tp % NEAR)
    near_lo = near % NEAR
    lo = tp % NEAR
    rows = skip_ref.shape[0]
    L = wq_ref.shape[0]
    H = L // 2
    group = n_tp * capp
    dense = cap >= rows and capp == rows
    inner = jnp.minimum(sp, n_sp - 1 - sp)

    def source(i):
        apart = (i + 1) // 2
        pair = jnp.where(i % 2 == 1, sp - apart, sp + apart)
        tail = jnp.where(sp == inner, sp + (i - inner), sp - (i - inner))
        return jnp.where(i <= 2 * inner, pair, tail)

    def al(i):
        return pl.multiple_of(i * capp, capp)

    weights = [
        pltpu.make_async_copy(wo_hbm, wo, wsem.at[0]),
        pltpu.make_async_copy(wg_hbm.at[0], wg, wsem.at[1]),
        pltpu.make_async_copy(wu_hbm.at[0], wu, wsem.at[2]),
        pltpu.make_async_copy(wd_hbm.at[0], wd, wsem.at[3]),
    ]
    for w in weights:
        w.start()

    barrier = pltpu.get_barrier_semaphore()
    for o in range(1, n_sp):
        pl.semaphore_signal(barrier, inc=1, device_id={"sp": (sp + o) % n_sp})
    for o in range(1, n_tp):
        pl.semaphore_signal(barrier, inc=1, device_id={"tp": (tp + o) % n_tp})

    lane = lax.broadcasted_iota(jnp.int32, (1, LANES), 1)
    first = lane < LANES // 2
    spk = [jnp.broadcast_to(spk_ref[h : h + 1, :], (LANES, L)).T for h in range(3)]
    spike = jnp.concatenate([spk[0], jnp.where(first, spk[1], spk[2])], axis=1)
    forget = jnp.concatenate([wf_ref[...], nf_ref[...]], axis=1).astype(F32)
    start = 1.0 / (1.0 + jnp.exp(forget))
    wq = wq_ref[...].astype(F32)
    nq = nq_ref[...].astype(F32)
    q = jnp.concatenate(
        [
            wq / (1.0 + jnp.exp(-wq)) * LANES**-0.5,
            nq / (1.0 + jnp.exp(-nq)) * (LANES // 2) ** -0.5,
        ],
        axis=1,
    )
    leak = jnp.concatenate([wl_ref[...], nl_ref[...]], axis=1)
    t_i = lax.broadcasted_iota(jnp.int32, (L, L), 0)
    s_i = lax.broadcasted_iota(jnp.int32, (L, L), 1)
    row = lax.broadcasted_iota(jnp.int32, (L, 1), 0)
    past = s_i <= t_i
    later = s_i >= t_i
    same = (t_i < H) == (s_i < H)
    v = v_ref[...]
    vs = [v[:, h * LANES : (h + 1) * LANES] for h in range(3)]
    ks, runs = [], []
    for d in range(2):
        k = leak[d : d + 1, :] * start
        a = jnp.log(1.0 - k) + spike
        tri = (past if d == 0 else later).astype(F32)
        run = lax.dot_general(
            tri,
            a,
            (((1,), (0,)), ((), ())),
            preferred_element_type=F32,
            precision=lax.Precision.HIGHEST,
        )
        total = run[L - 1 : L, :] if d == 0 else run[0:1, :]
        kk = (k * jnp.exp(total - run)).astype(BF16)
        wide = mm(vs[0], kk[:, :LANES], 0, 0)
        slim = jnp.where(first, mm(vs[1], kk[:, LANES:], 0, 0), mm(vs[2], kk[:, LANES:], 0, 0))
        st_out[d, :LANES, :] = jnp.concatenate([wide, slim], axis=1).astype(BF16)
        st_out[d, LANES:, :] = jnp.broadcast_to(
            total, (st_out.shape[1] - LANES, 2 * LANES)
        ).astype(BF16)
        ks.append(k)
        runs.append(run)

    pl.semaphore_wait(barrier, n_sp + n_tp - 2)

    def st_copy(o):
        dest = (sp + o) % n_sp
        way = (sp + o) // n_sp
        return pltpu.make_async_remote_copy(
            src_ref=st_out.at[way],
            dst_ref=st_in.at[sp],
            send_sem=st_ss.at[o],
            recv_sem=st_rs.at[sp],
            device_id={"sp": dest},
        )

    for o in range(1, n_sp):
        st_copy(o).start()

    outs = []
    scores = [None, None, None]
    for d in range(2):
        k, run = ks[d], runs[d]
        mid = jnp.where(row < H, run[H // 2 - 1 : H // 2, :], run[H + H // 2 - 1 : H + H // 2, :])
        edge = run[H - 1 : H, :] if d == 0 else run[H : H + 1, :]
        q_in = q * jnp.exp(run - mid)
        k_in = (k * jnp.exp(mid - run)).astype(BF16)
        q_off = q * jnp.exp(jnp.minimum(run - edge, 0.0))
        k_off = (k * jnp.exp(jnp.minimum(edge - run, 0.0))).astype(BF16)
        keep_in = same & (past if d == 0 else later)
        keep_off = ((t_i >= H) & (s_i < H)) if d == 0 else ((t_i < H) & (s_i >= H))
        for h in range(3):
            at = slice(0, LANES) if h == 0 else slice(LANES, 2 * LANES)
            qi, qo = q_in[:, at], q_off[:, at]
            if h > 0:
                mine = first if h == 1 else ~first
                qi, qo = jnp.where(mine, qi, 0.0), jnp.where(mine, qo, 0.0)
            part_in = jnp.where(keep_in, mm(qi.astype(BF16), k_in[:, at], 1, 1), 0.0)
            part_off = jnp.where(keep_off, mm(qo.astype(BF16), k_off[:, at], 1, 1), 0.0)
            both = part_in + part_off
            scores[h] = both if d == 0 else scores[h] + both
    for h in range(3):
        outs.append(mm(scores[h].astype(BF16), vs[h]))

    def take(src, state):
        pltpu.make_async_remote_copy(
            src_ref=st_out.at[0],
            dst_ref=st_in.at[src],
            send_sem=st_ss.at[0],
            recv_sem=st_rs.at[src],
            device_id={"sp": (sp + 1) % n_sp},
        ).wait_recv()
        got = st_in[src].astype(F32)
        return state * jnp.exp(got[LANES : LANES + 1, :]) + got[:LANES, :]

    zero = jnp.zeros((LANES, 2 * LANES), F32)
    ahead = lax.fori_loop(0, sp, take, zero)
    behind = lax.fori_loop(0, n_sp - 1 - sp, lambda i, s: take(n_sp - 1 - i, s), zero)
    for d, state in enumerate((ahead, behind)):
        state = state.astype(BF16)
        qd = q * jnp.exp(runs[d])
        for h in range(3):
            at = slice(0, LANES) if h == 0 else slice(LANES, 2 * LANES)
            qh = qd[:, at]
            if h > 0:
                qh = jnp.where(first if h == 1 else ~first, qh, 0.0)
            outs[h] = outs[h] + mm(qh.astype(BF16), state[:, at], 1, 1)
    g = gate_ref[...].astype(F32)
    g = g / (1.0 + jnp.exp(-g)) * chs_ref[...].reshape(1, -1)
    for h in range(3):
        at = slice(h * LANES, (h + 1) * LANES)
        o_h = outs[h]
        o_h = o_h * lax.rsqrt(jnp.mean(o_h * o_h, axis=1, keepdims=True) + EPS)
        y_s[:, at] = (o_h * g[:, at]).astype(BF16)

    weights[0].wait()
    y = y_s[...]
    D = wo.shape[1]
    step = D // 4
    for c in range(4):
        rs_out[:, c * step : (c + 1) * step] = mm(y, wo[:, c * step : (c + 1) * step]).astype(BF16)

    def rs_copy(o):
        dest = (tp + o) % n_tp
        return pltpu.make_async_remote_copy(
            src_ref=rs_out.at[pl.ds(pl.multiple_of(dest * rows, rows), rows)],
            dst_ref=rs_in.at[o - 1],
            send_sem=rs_ss.at[o - 1],
            recv_sem=rs_rs.at[o - 1],
            device_id={"tp": dest},
        )

    for o in range(1, n_tp):
        rs_copy(o).start()

    n_slot = n_sp * capp
    slot = lax.broadcasted_iota(jnp.int32, (n_slot, 1), 0)
    expert = jnp.zeros((n_slot, 1), jnp.int32)
    for e in range(1, n_sp):
        expert = expert + (slot >= e * capp).astype(jnp.int32)
    place = (slot - expert * capp).astype(F32)
    named = jnp.zeros((n_slot, rows), F32)
    share = jnp.zeros((n_slot, rows), F32)
    for c in range(asg_ref.shape[0]):
        hit = asg_ref[c : c + 1, :] == expert
        named = jnp.where(hit, 1.0, named)
        share = jnp.where(hit, shr_ref[c : c + 1, :], share)
    before = (
        lax.broadcasted_iota(jnp.int32, (rows, rows), 0)
        < lax.broadcasted_iota(jnp.int32, (rows, rows), 1)
    ).astype(BF16)
    if dense:
        count = lax.broadcasted_iota(jnp.int32, (n_slot, rows), 1).astype(F32)
    else:
        count = mm(named.astype(BF16), before)
    picked = jnp.where(count == place, named, 0.0)
    comb = picked * share
    comb_hi = comb.astype(BF16)
    comb_lo = (comb - comb_hi.astype(F32)).astype(BF16)

    total = skip_ref[...].astype(F32) + rs_out[pl.ds(pl.multiple_of(tp * rows, rows), rows), :].astype(F32)
    for o in range(1, n_tp):
        rs_copy(o).wait_recv()
        total = total + rs_in[o - 1].astype(F32)
    hid = total.astype(BF16)
    hid_s[...] = hid
    hf = hid.astype(F32)
    normed = (
        hf * lax.rsqrt(jnp.mean(hf * hf, axis=1, keepdims=True) + EPS) * nsc_ref[...]
    ).astype(BF16)
    if not dense:
        disp[...] = mm(picked.astype(BF16), normed).astype(BF16)

    def chunk(src, t):
        return al(src * n_tp + t)

    def z_copy(o):
        dest = (sp + o) % n_sp
        return pltpu.make_async_remote_copy(
            src_ref=disp.at[pl.ds(al(dest), capp)],
            dst_ref=xin.at[pl.ds(chunk(sp, tp), capp)],
            send_sem=z_ss.at[o, 0],
            recv_sem=ag_rs.at[sp, tp],
            device_id={"sp": dest},
        )

    def pass_on(src, up):
        at = pl.ds(chunk(src, tp), capp)
        return pltpu.make_async_remote_copy(
            src_ref=xin.at[at],
            dst_ref=xin.at[at],
            send_sem=z_ss.at[src, 0 if up else 1],
            recv_sem=ag_rs.at[src, tp],
            device_id={"sp": (sp + 1) % n_sp if up else (sp + n_sp - 1) % n_sp},
        )

    def pass_along(src, act):
        @pl.when((src <= sp) & (sp < n_sp - 1))
        def _():
            act(pass_on(src, True))

        @pl.when((src >= sp) & (sp > 0))
        def _():
            act(pass_on(src, False))

    if dense:
        xin[pl.ds(chunk(sp, tp), capp), :] = normed
        pass_along(sp, lambda c: c.start())
    else:
        for o in range(1, n_sp):
            z_copy(o).start()
        xin[pl.ds(chunk(sp, tp), capp), :] = disp[pl.ds(al(sp), capp), :]


    def tp_copy(src, t, sem, dest):
        return pltpu.make_async_remote_copy(
            src_ref=xin.at[pl.ds(chunk(src, t), capp)],
            dst_ref=xin.at[pl.ds(chunk(src, t), capp)],
            send_sem=sem,
            recv_sem=ag_rs.at[src, t],
            device_id={"tp": dest},
        )

    def far_copy(i, h):
        return tp_copy(source(i), tp, far_ss.at[i, h], (tp + NEAR * h) % n_tp)

    def near_copy(i, h):
        return tp_copy(source(i), (tp + NEAR * h) % n_tp, near_ss.at[i, h], near)

    def arrived(i, t):
        tp_copy(source(i), t, near_ss.at[i, 0], near).wait_recv()

    def spread(i):
        for h in range(1, n_hi):
            far_copy(i, h).start()
        near_copy(i, 0).start()

    def relay(i):
        for h in range(1, n_hi):
            arrived(i, (tp + NEAR * h) % n_tp)
            near_copy(i, h).start()

    def nr_copy(i, h):
        src = source(i)
        return pltpu.make_async_remote_copy(
            src_ref=part.at[pl.ds(chunk(src, h * NEAR + near_lo), capp)],
            dst_ref=nr_in.at[pl.ds(al(src * n_hi + h), capp)],
            send_sem=nr_ss.at[i, h],
            recv_sem=nr_rs.at[src, h],
            device_id={"tp": near},
        )

    def fr_copy(i, o):
        src = source(i)
        h = (hi + o) % n_hi
        return pltpu.make_async_remote_copy(
            src_ref=fr_out.at[pl.ds(al(src * n_hi + h), capp)],
            dst_ref=fr_in.at[pl.ds(al(src * n_hi + o), capp)],
            send_sem=fr_ss.at[i, o],
            recv_sem=fr_rs.at[src, o],
            device_id={"tp": (tp + NEAR * o) % n_tp},
        )

    def ret_copy(i):
        src = source(i)
        return pltpu.make_async_remote_copy(
            src_ref=fin.at[pl.ds(al(src), capp)],
            dst_ref=ret.at[pl.ds(al(sp), capp)],
            send_sem=ret_ss.at[i],
            recv_sem=ret_rs.at[sp],
            device_id={"sp": src},
        )

    def ffn(i):
        src = source(i)
        for h in range(n_hi):
            arrived(i, (near + NEAR * h) % n_tp)
        at = pl.multiple_of(src * group, group)
        x = xin[pl.ds(at, group), :]
        gp = mm(x, wg[...])
        up = mm(x, wu[...])
        act = (gp / (1.0 + jnp.exp(-gp)) * up).astype(BF16)
        for c in range(4):
            part[pl.ds(at, group), c * step : (c + 1) * step] = mm(
                act, wd[:, c * step : (c + 1) * step]
            ).astype(BF16)
        for h in range(n_hi):
            nr_copy(i, h).start()

    def near_sum(i):
        src = source(i)
        for o in range(1, n_hi + 1):
            h = (hi + o) % n_hi
            nr_copy(i, h).wait_recv()
            slot_at = pl.ds(al(src * n_hi + h), capp)
            fr_out[slot_at, :] = (
                part[pl.ds(chunk(src, h * NEAR + lo), capp), :].astype(F32)
                + nr_in[slot_at, :].astype(F32)
            ).astype(BF16)
            if o < n_hi:
                fr_copy(i, o).start()

    def far_sum(i):
        src = source(i)
        acc = fr_out[pl.ds(al(src * n_hi + hi), capp), :].astype(F32)
        for o in range(1, n_hi):
            fr_copy(i, o).wait_recv()
            acc = acc + fr_in[pl.ds(al(src * n_hi + o), capp), :].astype(F32)
        fin[pl.ds(al(src), capp), :] = acc.astype(BF16)

    def z_arrived(i):
        src = source(i)
        pltpu.make_async_remote_copy(
            src_ref=xin.at[pl.ds(chunk(src, tp), capp)],
            dst_ref=xin.at[pl.ds(chunk(src, tp), capp)],
            send_sem=z_ss.at[0, 0],
            recv_sem=ag_rs.at[src, tp],
            device_id={"sp": (sp + 1) % n_sp},
        ).wait_recv()
        if dense:
            pass_along(src, lambda c: c.start())
        spread(i)

    spread(0)
    relay(0)
    if n_sp > 1:
        z_arrived(1)
    if n_sp > 2:

        @pl.when(inner > 0)
        def _():
            z_arrived(2)

    for w in weights[1:]:
        w.wait()

    def body(i, carry):
        @pl.when(i < n_sp)
        def _():
            ffn(i)

        @pl.when((i + 2 < n_sp) & ((i > 0) | (inner == 0)))
        def _():
            z_arrived(i + 2)

        @pl.when(i + 1 < n_sp)
        def _():
            relay(i + 1)

        @pl.when(i < n_sp)
        def _():
            near_sum(i)

        @pl.when(i >= 1)
        def _():
            far_sum(i - 1)

        @pl.when(i >= 2)
        def _():
            ret_copy(i - 1).start()

        return carry

    lax.fori_loop(0, n_sp + 1, body, 0)

    ret[pl.ds(al(sp), capp), :] = fin[pl.ds(al(sp), capp), :]
    for o in range(1, n_sp):
        src = (sp + o) % n_sp
        pltpu.make_async_remote_copy(
            src_ref=fin.at[pl.ds(0, capp)],
            dst_ref=ret.at[pl.ds(al(src), capp)],
            send_sem=ret_ss.at[0],
            recv_sem=ret_rs.at[src],
            device_id={"sp": src},
        ).wait_recv()
    back = ret[...]
    out_ref[...] = (hid_s[...].astype(F32) + mm(comb_hi, back, 0, 0) + mm(comb_lo, back, 0, 0)).astype(BF16)

    for o in range(1, n_sp):
        st_copy(o).wait_send()
        if not dense:
            z_copy(o).wait_send()
        ret_copy(o).wait_send()
    for o in range(1, n_tp):
        rs_copy(o).wait_send()

    def drain(i, carry):
        if dense:
            pass_along(source(i), lambda c: c.wait_send())
        for h in range(1, n_hi):
            far_copy(i, h).wait_send()
            fr_copy(i, h).wait_send()
        for h in range(n_hi):
            near_copy(i, h).wait_send()
            nr_copy(i, h).wait_send()
        return carry

    lax.fori_loop(0, n_sp, drain, 0)


def local(n_sp, n_tp, *args):
    skip, wq = args[0], args[1]
    rows, D = skip.shape
    L = wq.shape[0]
    top = args[13].shape[1]
    cap = max(2, 2 * rows * top // n_sp)
    cap = min(cap, rows)
    capp = -(-cap // 16) * 16
    n_hi = n_tp // NEAR
    de = args[15].shape[2]
    heads = args[11].shape[0]
    args = list(args)
    for i in (9, 13, 14):
        args[i] = args[i].T
    args[12] = args[12].reshape(1, -1)
    vm = pl.BlockSpec(memory_space=pltpu.VMEM)
    hbm = pl.BlockSpec(memory_space=pl.ANY)
    specs = [hbm if i in (11, 15, 16, 17) else vm for i in range(len(args))]
    dma = pltpu.SemaphoreType.DMA
    scratch = [
        pltpu.VMEM((heads, D), BF16),
        pltpu.VMEM((D, de), BF16),
        pltpu.VMEM((D, de), BF16),
        pltpu.VMEM((de, D), BF16),
        pltpu.VMEM((2, LANES + 16, 2 * LANES), BF16),
        pltpu.VMEM((n_sp, LANES + 16, 2 * LANES), BF16),
        pltpu.VMEM((L, heads), BF16),
        pltpu.VMEM((L, D), BF16),
        pltpu.VMEM((n_tp - 1, rows, D), BF16),
        pltpu.VMEM((rows, D), BF16),
        pltpu.VMEM((n_sp * capp, D), BF16),
        pltpu.VMEM((n_sp * n_tp * capp, D), BF16),
        pltpu.VMEM((n_sp * n_tp * capp, D), BF16),
        pltpu.VMEM((n_sp * n_hi * capp, D), BF16),
        pltpu.VMEM((n_sp * n_hi * capp, D), BF16),
        pltpu.VMEM((n_sp * n_hi * capp, D), BF16),
        pltpu.VMEM((n_sp * capp, D), BF16),
        pltpu.VMEM((n_sp * capp, D), BF16),
        dma((4,)),
        dma((n_sp,)),
        dma((n_sp,)),
        dma((n_tp - 1,)),
        dma((n_tp - 1,)),
        dma((n_sp, 2)),
        dma((n_sp, n_hi)),
        dma((n_sp, n_hi)),
        dma((n_sp, n_tp)),
        dma((n_sp, n_hi)),
        dma((n_sp, n_hi)),
        dma((n_sp, n_hi)),
        dma((n_sp, n_hi)),
        dma((n_sp,)),
        dma((n_sp,)),
    ]
    return pl.pallas_call(
        functools.partial(kernel, n_sp, n_tp, cap, capp),
        out_shape=jax.ShapeDtypeStruct((rows, D), BF16),
        in_specs=specs,
        out_specs=vm,
        scratch_shapes=scratch,
        compiler_params=pltpu.CompilerParams(
            collective_id=0, has_side_effects=True, vmem_limit_bytes=60 * 1024 * 1024
        ),
    )(*args)


def solution(mesh):
    placed = (
        P(("grp", "sp", "tp"), None),
        P(("grp", "sp"), "tp"),
        P(("grp", "sp"), "tp"),
        P(("grp", "sp"), "tp"),
        P(("grp", "sp"), "tp"),
        P(None, "tp"),
        P(None, "tp"),
        P(("grp", "sp"), "tp"),
        P(("grp", "sp"), "tp"),
        P(("grp", "sp"), "tp"),
        P("tp"),
        P("tp", None),
        P(),
        P(("grp", "sp", "tp"), None),
        P(("grp", "sp", "tp"), None),
        P("sp", None, "tp"),
        P("sp", None, "tp"),
        P("sp", "tp", None),
    )
    return jax.shard_map(
        functools.partial(local, mesh.shape["sp"], mesh.shape["tp"]),
        mesh=mesh,
        in_specs=placed,
        out_specs=P(("grp", "sp", "tp"), None),
        check_vma=False,
    )
```
